32 devices in a mesh: grp: 2 (over y), sp: 4 (over z), tp: 4 (over x, core).
Axes of the slice: x: 2, y: 2, z: 4, core: 2. Of those that a mesh axis runs over, the one named last changes fastest.
Arguments:
- tokens: bfloat16 [8, 1024, 2048], P('grp', 'sp'), parts along dimension 0, may hold values from -6 to 6
- norm_gain: bfloat16 [2048], replicated, may hold values from 0.099609375 to 1.8984375
- key_weight: bfloat16 [2048, 2048], P(None, 'tp'), may hold values from -0.125 to 0.125
- value_weight: bfloat16 [2048, 2048], P(None, 'tp'), may hold values from -0.125 to 0.125
- break_bias: bfloat16 [8, 1024, 16], P('grp', 'sp', 'tp'), parts along dimension 0, may hold values from -12 to 0
- new_query: bfloat16 [8, 2048], P('grp', 'tp'), parts along dimension 0, may hold values from -6 to 6
Outputs:
- cache_pair: bfloat16 [8, 4, 256, 2, 2048], P(('grp', 'sp'), None, None, None, 'tp'), parts along dimension 0
- cache_bias: bfloat16 [8, 4, 256, 16], P(('grp', 'sp'), None, None, 'tp'), parts along dimension 0
- attended: float32 [8, 2048], P('grp', 'tp'), parts along dimension 0
The draws below stay inside these ranges and needn't reach their ends.
There are 2 independent parts, one for each index of `grp`. The reference program is written for one: setup_inputs(seed, part) draws one part's arguments, and reference() takes and returns one part's arrays. A program takes and returns all parts, laid end to end along the dimension named above; an argument that names none is the same for every part. Nothing has to cross between parts.
All inputs are finite; a program needn't handle non-finite values.
Results may differ from the reference program's by a relative error of at most 0.0064.
Values may be sent and summed in bfloat16 or wider, within the bound.
No kernel may reach another device: no remote copies, remote signals or barrier semaphores. Data moves between devices by JAX's collectives and lax.ppermute only.
A program may use at most 64 MiB of HBM per device.

```python
import jax
import jax.numpy as jnp
from jax import lax

D = 2048
HEADS = 16
DH = 128
SEQS = 4
PROMPT_LENGTH = 1024
SPAN = 1
PIECE = 256
N_SP = 4


def draw_break_bias(key, part):
    key_sequence = jax.random.split(key, 6)
    complete_shape = (SEQS, PROMPT_LENGTH, HEADS)
    kind_draw = jax.random.uniform(key_sequence[0], (SEQS, 1, HEADS))
    fast_share = 0.5
    slow_rate = jnp.exp(jax.random.uniform(key_sequence[1], (SEQS, 1, HEADS), minval=jnp.log(0.3), maxval=jnp.log(0.8))) / PROMPT_LENGTH
    fast_rate = jnp.exp(jax.random.uniform(key_sequence[2], (SEQS, 1, HEADS), minval=jnp.log(0.01), maxval=jnp.log(1.0 / 30.0)))
    decay_rate = jnp.where(kind_draw < fast_share, fast_rate, slow_rate)
    block_multiplier = jax.random.uniform(key_sequence[3], (SEQS, 32, 1, HEADS), minval=-0.7, maxval=0.7)
    block_multiplier = jnp.broadcast_to(block_multiplier, (SEQS, 32, PROMPT_LENGTH // 32, HEADS)).reshape(complete_shape)
    constant_level = jnp.log(decay_rate) + block_multiplier
    spike_marker = jax.random.uniform(key_sequence[4], complete_shape) < 4.0 / PROMPT_LENGTH
    spike_threshold = jax.random.uniform(key_sequence[5], complete_shape, minval=-1.4, maxval=0.0)
    return jnp.where(spike_marker, spike_threshold, constant_level).astype(jnp.bfloat16)


def level_of(rng, shape, shards, least, top_value):
    loudness = 1.0
    for axis_at, parts in shards:
        draws = jax.random.uniform(jax.random.fold_in(jax.random.fold_in(rng, 6), axis_at), (parts,), jnp.float32, least / len(shards), top_value / len(shards))
        loudness = loudness * jnp.repeat(jnp.exp(draws), shape[axis_at] // parts).reshape((-1,) + (1,) * (len(shape) - 1 - axis_at))
    return loudness


def centred(rng, shape, scale, most, cuts=(), dtype=jnp.bfloat16):
    array = scale * jax.random.normal(rng, shape, jnp.float32)
    if cuts:
        array = array * level_of(rng, shape, cuts, -0.22, 0.18)
    return jnp.clip(array, -most, most).astype(dtype)


def setup_inputs(seed: int = 0, part: int = 0) -> dict:
    keys = jax.random.split(jax.random.key(seed), 7)
    own_keys = jax.random.split(jax.random.fold_in(keys[6], part), 7)
    return {
        "tokens": centred(own_keys[0], (SEQS, PROMPT_LENGTH, D), 1.0, 6.0, ((1, 4),)),
        "norm_gain": jnp.clip(1.0 + 0.18 * jax.random.normal(keys[1], (D,), jnp.float32), 0.099609375, 1.8984375).astype(jnp.bfloat16),
        "key_weight": centred(keys[2], (D, HEADS * DH), D ** -0.5, 0.125, ((1, 4),)),
        "value_weight": centred(keys[3], (D, HEADS * DH), D ** -0.5, 0.125, ((1, 4),)),
        "break_bias": draw_break_bias(jax.random.fold_in(jax.random.fold_in(keys[6], part), 71), part),
        "new_query": centred(own_keys[5], (SEQS, HEADS * DH), 1.0, 6.0, ((1, 4),)),
    }


norm_eps = 1e-06

def arrange(rows, width):
    shaped = rows.reshape(SEQS, N_SP, SPAN, PIECE, width)
    shaped = jnp.transpose(shaped, (0, 2, 1, 3, 4))
    return shaped.reshape(SEQS * SPAN, N_SP, PIECE, width)

def reference(tokens, norm_gain, key_weight, value_weight, break_bias, new_query):
    widened = tokens.astype(jnp.float32)
    inverse = lax.rsqrt(lax.optimization_barrier(jnp.mean(widened * widened, axis=-1, keepdims=True)) + norm_eps)
    normed = (widened * inverse * norm_gain.astype(jnp.float32)).astype(jnp.bfloat16)
    flat_rows = normed.reshape(SEQS * PROMPT_LENGTH, D)
    key_rows = jnp.dot(flat_rows, key_weight, preferred_element_type=jnp.float32).astype(jnp.bfloat16)
    value_rows = jnp.dot(flat_rows, value_weight, preferred_element_type=jnp.float32).astype(jnp.bfloat16)
    key_rows = key_rows.reshape(SEQS, PROMPT_LENGTH, HEADS * DH)
    value_rows = value_rows.reshape(SEQS, PROMPT_LENGTH, HEADS * DH)
    cache_pair = jnp.stack((arrange(key_rows, HEADS * DH), arrange(value_rows, HEADS * DH)), axis=3)
    cache_bias = arrange(break_bias, HEADS)
    queries = new_query.reshape(SEQS, HEADS, DH).astype(jnp.float32)
    key_heads = key_rows.reshape(SEQS, PROMPT_LENGTH, HEADS, DH).astype(jnp.float32)
    value_heads = value_rows.reshape(SEQS, PROMPT_LENGTH, HEADS, DH).astype(jnp.float32)
    logits = jnp.einsum('shd,sphd->sph', queries, key_heads)
    logits = logits * DH ** (-0.5) + break_bias.astype(jnp.float32)
    keep_log = jax.nn.log_sigmoid(-logits)
    later_sum = lax.cumsum(keep_log, axis=1, reverse=True) - keep_log
    stick_weights = jnp.exp(jax.nn.log_sigmoid(logits) + later_sum).astype(jnp.bfloat16)
    attended = jnp.einsum('sph,sphd->shd', stick_weights.astype(jnp.float32), value_heads)
    return (cache_pair, cache_bias, attended.reshape(SEQS, HEADS * DH))
```

```python
import functools

import jax
import jax.numpy as jnp
from jax import lax
from jax.experimental import pallas as pl
from jax.experimental.pallas import tpu as pltpu
from jax.sharding import PartitionSpec as P

norm_eps = 1e-06


def normalize(tokens, norm_gain):
    widened = tokens.astype(jnp.float32)
    inverse = lax.rsqrt(jnp.mean(widened * widened, axis=-1, keepdims=True) + norm_eps)
    return (widened * inverse * norm_gain.astype(jnp.float32)).astype(jnp.bfloat16)


def project(flat_rows, key_weight, value_weight):
    key_rows = jnp.dot(flat_rows, key_weight, preferred_element_type=jnp.float32).astype(
        jnp.bfloat16
    )
    value_rows = jnp.dot(flat_rows, value_weight, preferred_element_type=jnp.float32).astype(
        jnp.bfloat16
    )
    return (key_rows, value_rows)


def read_placed(new_query, key_rows, value_rows, bias_rows, seq_count):
    block_count, piece, heads_here = bias_rows.shape
    columns = key_rows.shape[2]
    head_size = columns // heads_here
    span = block_count // seq_count
    own_index = lax.axis_index("sp")
    own_seq = own_index // span
    own_part = own_index % span
    own_query = lax.dynamic_slice_in_dim(new_query, own_seq, 1, 0).reshape(heads_here, head_size)
    key_heads = key_rows.reshape(block_count, piece, heads_here, head_size)
    logits = jnp.einsum("hd,nphd->nph", own_query, key_heads, preferred_element_type=jnp.float32)
    logits = logits * head_size ** (-0.5) + bias_rows.astype(jnp.float32)
    keep_log = jax.nn.log_sigmoid(-logits)
    block_totals = jnp.sum(keep_log, axis=1)
    own_slot = (jnp.arange(block_count, dtype=jnp.int32) == own_index)[:, None, None]
    placed = jnp.where(own_slot, block_totals[None], 0.0)
    gathered = lax.psum(placed, "sp")
    same_prompt = lax.dynamic_slice_in_dim(gathered, own_seq * span, span, 0)
    ordered = jnp.transpose(same_prompt, (1, 0, 2)).reshape(block_count * span, heads_here)
    beyond = lax.cumsum(ordered, axis=0, reverse=True) - ordered
    beyond = beyond.reshape(block_count, span, heads_here)
    carried = lax.dynamic_slice_in_dim(beyond, own_part, 1, 1)[:, 0, :]
    later_sum = lax.cumsum(keep_log, axis=1, reverse=True) - keep_log + carried[:, None, :]
    stick_weights = jnp.exp(jax.nn.log_sigmoid(logits) + later_sum).astype(jnp.bfloat16)
    value_heads = value_rows.reshape(block_count, piece, heads_here, head_size)
    mixed = jnp.einsum(
        "nph,nphd->hd", stick_weights, value_heads, preferred_element_type=jnp.float32
    )
    chosen = (jnp.arange(seq_count, dtype=jnp.int32) == own_seq)[:, None]
    partial_rows = jnp.where(chosen, mixed.reshape(1, columns), 0.0)
    return lax.psum(partial_rows, "sp")


def exchange_rows(tokens, norm_gain, key_weight, value_weight, break_bias, new_query):
    seq_count, tok_rows, width = tokens.shape
    heads_here = break_bias.shape[2]
    block_count = lax.axis_size("sp")
    piece = tok_rows * seq_count // block_count
    columns = key_weight.shape[1]
    normed = normalize(tokens, norm_gain)
    bias_pieces = break_bias.reshape(block_count, piece, heads_here)
    key_rows, value_rows = project(normed.reshape(-1, width), key_weight, value_weight)
    stacked_rows = jnp.stack((key_rows, value_rows), axis=1).reshape(block_count, piece, 2, columns)
    paired, bias_arrived = (
        lax.all_to_all(stacked_rows, "sp", split_axis=0, concat_axis=0, tiled=True),
        lax.all_to_all(bias_pieces, "sp", split_axis=0, concat_axis=0, tiled=True),
    )
    key_rows = paired[:, :, 0]
    value_rows = paired[:, :, 1]
    attended = read_placed(new_query, key_rows, value_rows, bias_arrived, seq_count)
    return (paired[None], bias_arrived[None], attended)


def block_kernel(part_count, whole_rows, carried, *refs):
    index_ref = refs[0]
    parts = refs[1 : 1 + part_count]
    gain_ref, key_ref, value_ref, bias_ref, query_ref = refs[1 + part_count : 6 + part_count]
    rest = refs[6 + part_count + (2 if carried else 0) :]
    cache_ref, bias_out_ref, partial_ref, total_ref, normed_ref = rest
    piece, width = normed_ref.shape
    heads_here = bias_ref.shape[-2]
    columns = key_ref.shape[1]
    head_size = columns // heads_here
    gain = gain_ref[...].astype(jnp.float32)
    if whole_rows:
        widened = parts[0][0].astype(jnp.float32)
        square_sum = jnp.sum(widened * widened, axis=-1, keepdims=True)
        inverse = lax.rsqrt(square_sum * (1.0 / width) + norm_eps)
        normed_ref[...] = (widened * inverse * gain).astype(jnp.bfloat16)
    else:
        share = width // part_count
        square_sum = jnp.zeros((piece, 1), jnp.float32)
        for part in parts:
            widened = part[...].astype(jnp.float32)
            square_sum = square_sum + jnp.sum(widened * widened, axis=-1, keepdims=True)
        inverse = lax.rsqrt(square_sum * (1.0 / width) + norm_eps)
        for offset, part in enumerate(parts):
            start = pl.multiple_of((index_ref[1] ^ offset) * share, share)
            own_gain = gain_ref[:, pl.ds(start, share)].astype(jnp.float32)
            scaled = part[...].astype(jnp.float32) * inverse * own_gain
            normed_ref[:, pl.ds(start, share)] = scaled.astype(jnp.bfloat16)
    normed = normed_ref[...]
    key_rows = jnp.dot(normed, key_ref[...], preferred_element_type=jnp.float32).astype(
        jnp.bfloat16
    )
    value_rows = jnp.dot(normed, value_ref[...], preferred_element_type=jnp.float32).astype(
        jnp.bfloat16
    )
    cache_ref[0, 0] = jnp.stack((key_rows, value_rows), axis=1)
    bias = bias_ref[...].reshape(heads_here, piece)
    bias_out_ref[0] = bias
    head_of_row = lax.broadcasted_iota(jnp.int32, (heads_here, columns), 0)
    head_of_column = lax.broadcasted_iota(jnp.int32, (heads_here, columns), 1) // head_size
    own_head = head_of_row == head_of_column
    query = jnp.where(own_head, query_ref[...], 0.0).astype(jnp.bfloat16)
    logits = lax.dot_general(
        query, key_rows, (((1,), (1,)), ((), ())), preferred_element_type=jnp.float32
    )
    logits = logits * head_size ** (-0.5) + bias.astype(jnp.float32)
    soft = jnp.log1p(jnp.exp(-jnp.abs(logits)))
    keep_log = jnp.minimum(-logits, 0.0) - soft
    break_log = jnp.minimum(logits, 0.0) - soft
    earlier = lax.broadcasted_iota(jnp.int32, (piece, piece), 1)
    later = lax.broadcasted_iota(jnp.int32, (piece, piece), 0) > earlier
    later_sum = jnp.dot(
        keep_log,
        later.astype(jnp.float32),
        preferred_element_type=jnp.float32,
        precision=lax.Precision.HIGHEST,
    )
    weights = jnp.exp(break_log + later_sum).astype(jnp.bfloat16)
    mixed = jnp.dot(weights, value_rows, preferred_element_type=jnp.float32)
    partial_ref[...] = jnp.sum(jnp.where(own_head, mixed, 0.0), axis=0, keepdims=True)
    totals = jnp.sum(keep_log, axis=1, keepdims=True)
    total_ref[...] = jnp.sum(jnp.where(own_head, totals, 0.0), axis=0, keepdims=True)


def build_block(index, parts, gain, key_weight, value_weight, bias, query, carried, block_count):
    whole_rows = parts[0].ndim == 3
    width, columns = key_weight.shape
    piece = parts[0].shape[-2]
    heads_here = bias.shape[-2]
    part_count = len(parts)

    def full(array):
        return pl.BlockSpec(array.shape, lambda g, s: (0,) * array.ndim)

    if whole_rows:
        part_specs = [pl.BlockSpec((1, piece, width), lambda g, s: (s[0], 0, 0))]
        bias_spec = pl.BlockSpec((1, heads_here, piece), lambda g, s: (s[0], 0, 0))
    else:
        part_specs = [full(part) for part in parts]
        bias_spec = full(bias)
    operands = [index, *parts, gain, key_weight, value_weight, bias, query]
    specs = part_specs + [full(gain), full(key_weight), full(value_weight), bias_spec, full(query)]
    aliases = {}
    if carried is not None:
        aliases = {len(operands): 0, len(operands) + 1: 1}
        operands += list(carried)
        specs += [pl.BlockSpec(memory_space=pl.ANY)] * 2
    row = jax.ShapeDtypeStruct((1, columns), jnp.float32)
    return pl.pallas_call(
        functools.partial(block_kernel, part_count, whole_rows, carried is not None),
        grid_spec=pltpu.PrefetchScalarGridSpec(
            num_scalar_prefetch=1,
            grid=(1,),
            in_specs=specs,
            out_specs=[
                pl.BlockSpec((1, 1, piece, 2, columns), lambda g, s: (0, s[0], 0, 0, 0)),
                pl.BlockSpec((1, heads_here, piece), lambda g, s: (s[0], 0, 0)),
                pl.BlockSpec((1, columns), lambda g, s: (0, 0)),
                pl.BlockSpec((1, columns), lambda g, s: (0, 0)),
            ],
            scratch_shapes=[pltpu.VMEM((piece, width), jnp.bfloat16)],
        ),
        out_shape=[
            jax.ShapeDtypeStruct((1, block_count, piece, 2, columns), jnp.bfloat16),
            jax.ShapeDtypeStruct((block_count, heads_here, piece), jnp.bfloat16),
            row,
            row,
        ],
        input_output_aliases=aliases,
    )(*operands)


def swap(array, axis, offset):
    size = lax.axis_size(axis)
    return lax.ppermute(array, axis, [(k, k ^ offset) for k in range(size)])


def exchange_order(size):
    return [1] + list(range(size - 1, 1, -1))


def exchange_tokens(tokens, norm_gain, key_weight, value_weight, break_bias, new_query):
    seq_count, piece, width = tokens.shape
    block_count = lax.axis_size("sp")
    share_count = lax.axis_size("tp")
    share = width // share_count
    own = lax.axis_index("sp")
    own_share = lax.axis_index("tp")
    bias_rows = jnp.transpose(break_bias, (0, 2, 1))
    heads_here = bias_rows.shape[1]
    columns = key_weight.shape[1]
    gain = norm_gain.reshape(1, width)
    query = lax.dynamic_slice_in_dim(new_query, own, 1, 0).astype(jnp.float32)

    def index_of(offset):
        return jnp.stack((own ^ offset, own_share)).astype(jnp.int32)

    order = exchange_order(block_count)
    arrived = {}
    bias_arrived = {}
    for offset in order:
        sent = lax.dynamic_slice(
            tokens, (own ^ offset, 0, own_share * share), (1, piece, share)
        ).reshape(piece, share)
        arrived[offset] = swap(sent, "sp", offset)
    for offset in order:
        bias_sent = lax.dynamic_index_in_dim(bias_rows, own ^ offset, 0, False)
        bias_arrived[offset] = swap(bias_sent, "sp", offset)
    built = {}
    built[0] = build_block(
        index_of(0), [tokens], gain, key_weight, value_weight, bias_rows, query, None, block_count
    )
    latest = built[0]
    for offset in order:
        shares = {0: arrived[offset]}
        bit = share_count // 2
        while bit:
            for known in list(shares):
                shares[known | bit] = swap(shares[known], "tp", bit)
            bit //= 2
        parts = [shares[k] for k in range(share_count)]
        latest = build_block(
            index_of(offset),
            parts,
            gain,
            key_weight,
            value_weight,
            bias_arrived[offset],
            query,
            latest[:2],
            block_count,
        )
        built[offset] = latest
    cache_pair, cache_bias = latest[:2]
    attended = jnp.zeros((1, columns), jnp.float32)
    for offset, block in built.items():
        beyond = jnp.zeros((1, columns), jnp.float32)
        for other, other_block in built.items():
            if other != offset:
                beyond = beyond + jnp.where((own ^ other) > (own ^ offset), other_block[3], 0.0)
        attended = attended + block[2] * jnp.exp(beyond)
    seq_index = lax.broadcasted_iota(jnp.int32, (seq_count, 1), 0)
    gathered = jnp.where(seq_index == own, attended, 0.0)
    for offset in order:
        gathered = jnp.where(seq_index == (own ^ offset), swap(attended, "sp", offset), gathered)
    return (cache_pair, jnp.transpose(cache_bias, (0, 2, 1))[None], gathered)


def local(tokens, norm_gain, key_weight, value_weight, break_bias, new_query):
    seq_count, _, width = tokens.shape
    block_count = lax.axis_size("sp")
    share_count = lax.axis_size("tp")
    paired = block_count & (block_count - 1) == 0 and share_count & (share_count - 1) == 0
    aligned = width % (128 * share_count) == 0
    whole_prompt = seq_count == block_count and block_count > 1
    body = exchange_tokens if paired and aligned and whole_prompt else exchange_rows
    return body(tokens, norm_gain, key_weight, value_weight, break_bias, new_query)


def solution(mesh):
    return jax.shard_map(
        local,
        mesh=mesh,
        in_specs=(
            P("grp", "sp", None),
            P(),
            P(None, "tp"),
            P(None, "tp"),
            P("grp", "sp", "tp"),
            P("grp", "tp"),
        ),
        out_specs=(
            P(("grp", "sp"), None, None, None, "tp"),
            P(("grp", "sp"), None, None, "tp"),
            P("grp", "tp"),
        ),
        check_vma=False,
    )
```

```python
import functools

import jax
import jax.numpy as jnp
from jax import lax
from jax.experimental import pallas as pl
from jax.experimental.pallas import tpu as pltpu
from jax.sharding import PartitionSpec as P

norm_eps = 1e-06


def normalize(tokens, norm_gain):
    widened = tokens.astype(jnp.float32)
    inverse = lax.rsqrt(jnp.mean(widened * widened, axis=-1, keepdims=True) + norm_eps)
    return (widened * inverse * norm_gain.astype(jnp.float32)).astype(jnp.bfloat16)


def project(flat_rows, key_weight, value_weight):
    key_rows = jnp.dot(flat_rows, key_weight, preferred_element_type=jnp.float32).astype(
        jnp.bfloat16
    )
    value_rows = jnp.dot(flat_rows, value_weight, preferred_element_type=jnp.float32).astype(
        jnp.bfloat16
    )
    return (key_rows, value_rows)


def read_placed(new_query, key_rows, value_rows, bias_rows, seq_count):
    block_count, piece, heads_here = bias_rows.shape
    columns = key_rows.shape[2]
    head_size = columns // heads_here
    span = block_count // seq_count
    own_index = lax.axis_index("sp")
    own_seq = own_index // span
    own_part = own_index % span
    own_query = lax.dynamic_slice_in_dim(new_query, own_seq, 1, 0).reshape(heads_here, head_size)
    key_heads = key_rows.reshape(block_count, piece, heads_here, head_size)
    logits = jnp.einsum("hd,nphd->nph", own_query, key_heads, preferred_element_type=jnp.float32)
    logits = logits * head_size ** (-0.5) + bias_rows.astype(jnp.float32)
    keep_log = jax.nn.log_sigmoid(-logits)
    block_totals = jnp.sum(keep_log, axis=1)
    own_slot = (jnp.arange(block_count, dtype=jnp.int32) == own_index)[:, None, None]
    placed = jnp.where(own_slot, block_totals[None], 0.0)
    gathered = lax.psum(placed, "sp")
    same_prompt = lax.dynamic_slice_in_dim(gathered, own_seq * span, span, 0)
    ordered = jnp.transpose(same_prompt, (1, 0, 2)).reshape(block_count * span, heads_here)
    beyond = lax.cumsum(ordered, axis=0, reverse=True) - ordered
    beyond = beyond.reshape(block_count, span, heads_here)
    carried = lax.dynamic_slice_in_dim(beyond, own_part, 1, 1)[:, 0, :]
    later_sum = lax.cumsum(keep_log, axis=1, reverse=True) - keep_log + carried[:, None, :]
    stick_weights = jnp.exp(jax.nn.log_sigmoid(logits) + later_sum).astype(jnp.bfloat16)
    value_heads = value_rows.reshape(block_count, piece, heads_here, head_size)
    mixed = jnp.einsum(
        "nph,nphd->hd", stick_weights, value_heads, preferred_element_type=jnp.float32
    )
    chosen = (jnp.arange(seq_count, dtype=jnp.int32) == own_seq)[:, None]
    partial_rows = jnp.where(chosen, mixed.reshape(1, columns), 0.0)
    return lax.psum(partial_rows, "sp")


def exchange_rows(tokens, norm_gain, key_weight, value_weight, break_bias, new_query):
    seq_count, tok_rows, width = tokens.shape
    heads_here = break_bias.shape[2]
    block_count = lax.axis_size("sp")
    piece = tok_rows * seq_count // block_count
    columns = key_weight.shape[1]
    normed = normalize(tokens, norm_gain)
    bias_pieces = break_bias.reshape(block_count, piece, heads_here)
    key_rows, value_rows = project(normed.reshape(-1, width), key_weight, value_weight)
    stacked_rows = jnp.stack((key_rows, value_rows), axis=1).reshape(block_count, piece, 2, columns)
    paired, bias_arrived = (
        lax.all_to_all(stacked_rows, "sp", split_axis=0, concat_axis=0, tiled=True),
        lax.all_to_all(bias_pieces, "sp", split_axis=0, concat_axis=0, tiled=True),
    )
    key_rows = paired[:, :, 0]
    value_rows = paired[:, :, 1]
    attended = read_placed(new_query, key_rows, value_rows, bias_arrived, seq_count)
    return (paired[None], bias_arrived[None], attended)


def block_kernel(part_count, whole_rows, carried, *refs):
    index_ref = refs[0]
    parts = refs[1 : 1 + part_count]
    gain_ref, key_ref, value_ref, bias_ref, query_ref = refs[1 + part_count : 6 + part_count]
    rest = refs[6 + part_count + (2 if carried else 0) :]
    cache_ref, bias_out_ref, partial_ref, total_ref = rest[:4]
    normed_ref, key_local, value_local, weight_sems = rest[4:]
    key_copy = pltpu.make_async_copy(key_ref, key_local, weight_sems.at[0])
    value_copy = pltpu.make_async_copy(value_ref, value_local, weight_sems.at[1])
    key_copy.start()
    value_copy.start()
    piece, width = normed_ref.shape
    heads_here = bias_ref.shape[-2]
    columns = key_ref.shape[1]
    head_size = columns // heads_here
    gain = gain_ref[...].astype(jnp.float32)
    if whole_rows:
        widened = parts[0][0].astype(jnp.float32)
        square_sum = jnp.sum(widened * widened, axis=-1, keepdims=True)
        inverse = lax.rsqrt(square_sum * (1.0 / width) + norm_eps)
        normed_ref[...] = (widened * inverse * gain).astype(jnp.bfloat16)
    else:
        share = width // part_count
        square_sum = jnp.zeros((piece, 1), jnp.float32)
        for part in parts:
            widened = part[...].astype(jnp.float32)
            square_sum = square_sum + jnp.sum(widened * widened, axis=-1, keepdims=True)
        inverse = lax.rsqrt(square_sum * (1.0 / width) + norm_eps)
        for offset, part in enumerate(parts):
            start = pl.multiple_of((index_ref[1] ^ offset) * share, share)
            own_gain = gain_ref[:, pl.ds(start, share)].astype(jnp.float32)
            scaled = part[...].astype(jnp.float32) * inverse * own_gain
            normed_ref[:, pl.ds(start, share)] = scaled.astype(jnp.bfloat16)
    normed = normed_ref[...]
    key_copy.wait()
    key_rows = jnp.dot(normed, key_local[...], preferred_element_type=jnp.float32).astype(
        jnp.bfloat16
    )
    value_copy.wait()
    value_rows = jnp.dot(normed, value_local[...], preferred_element_type=jnp.float32).astype(
        jnp.bfloat16
    )
    cache_ref[0, 0] = jnp.stack((key_rows, value_rows), axis=1)
    bias = bias_ref[...].reshape(heads_here, piece)
    bias_out_ref[0] = bias
    head_of_row = lax.broadcasted_iota(jnp.int32, (heads_here, columns), 0)
    head_of_column = lax.broadcasted_iota(jnp.int32, (heads_here, columns), 1) // head_size
    own_head = head_of_row == head_of_column
    query = jnp.where(own_head, query_ref[...], 0.0).astype(jnp.bfloat16)
    logits = lax.dot_general(
        query, key_rows, (((1,), (1,)), ((), ())), preferred_element_type=jnp.float32
    )
    logits = logits * head_size ** (-0.5) + bias.astype(jnp.float32)
    soft = jnp.log1p(jnp.exp(-jnp.abs(logits)))
    keep_log = jnp.minimum(-logits, 0.0) - soft
    break_log = jnp.minimum(logits, 0.0) - soft
    earlier = lax.broadcasted_iota(jnp.int32, (piece, piece), 1)
    later = lax.broadcasted_iota(jnp.int32, (piece, piece), 0) > earlier
    later_sum = jnp.dot(
        keep_log,
        later.astype(jnp.float32),
        preferred_element_type=jnp.float32,
        precision=lax.Precision.HIGHEST,
    )
    weights = jnp.exp(break_log + later_sum).astype(jnp.bfloat16)
    mixed = jnp.dot(weights, value_rows, preferred_element_type=jnp.float32)
    partial_ref[...] = jnp.sum(jnp.where(own_head, mixed, 0.0), axis=0, keepdims=True)
    totals = jnp.sum(keep_log, axis=1, keepdims=True)
    total_ref[...] = jnp.sum(jnp.where(own_head, totals, 0.0), axis=0, keepdims=True)


def build_block(index, parts, gain, key_weight, value_weight, bias, query, carried, block_count):
    whole_rows = parts[0].ndim == 3
    width, columns = key_weight.shape
    piece = parts[0].shape[-2]
    heads_here = bias.shape[-2]
    part_count = len(parts)

    def full(array):
        return pl.BlockSpec(array.shape, lambda g, s: (0,) * array.ndim)

    if whole_rows:
        part_specs = [pl.BlockSpec((1, piece, width), lambda g, s: (s[0], 0, 0))]
        bias_spec = pl.BlockSpec((1, heads_here, piece), lambda g, s: (s[0], 0, 0))
    else:
        part_specs = [full(part) for part in parts]
        bias_spec = full(bias)
    operands = [index, *parts, gain, key_weight, value_weight, bias, query]
    in_place = pl.BlockSpec(memory_space=pl.ANY)
    specs = part_specs + [full(gain), in_place, in_place, bias_spec, full(query)]
    aliases = {}
    if carried is not None:
        aliases = {len(operands): 0, len(operands) + 1: 1}
        operands += list(carried)
        specs += [in_place] * 2
    row = jax.ShapeDtypeStruct((1, columns), jnp.float32)
    return pl.pallas_call(
        functools.partial(block_kernel, part_count, whole_rows, carried is not None),
        grid_spec=pltpu.PrefetchScalarGridSpec(
            num_scalar_prefetch=1,
            grid=(1,),
            in_specs=specs,
            out_specs=[
                pl.BlockSpec((1, 1, piece, 2, columns), lambda g, s: (0, s[0], 0, 0, 0)),
                pl.BlockSpec((1, heads_here, piece), lambda g, s: (s[0], 0, 0)),
                pl.BlockSpec((1, columns), lambda g, s: (0, 0)),
                pl.BlockSpec((1, columns), lambda g, s: (0, 0)),
            ],
            scratch_shapes=[
                pltpu.VMEM((piece, width), jnp.bfloat16),
                pltpu.VMEM((width, columns), jnp.bfloat16),
                pltpu.VMEM((width, columns), jnp.bfloat16),
                pltpu.SemaphoreType.DMA((2,)),
            ],
        ),
        out_shape=[
            jax.ShapeDtypeStruct((1, block_count, piece, 2, columns), jnp.bfloat16),
            jax.ShapeDtypeStruct((block_count, heads_here, piece), jnp.bfloat16),
            row,
            row,
        ],
        input_output_aliases=aliases,
        cost_estimate=pl.CostEstimate(
            flops=4 * piece * width * columns,
            transcendentals=3 * heads_here * piece,
            bytes_accessed=4 * width * columns + 2 * piece * (width + 2 * columns),
        ),
    )(*operands)


def swap(array, axis, offset):
    size = lax.axis_size(axis)
    return lax.ppermute(array, axis, [(k, k ^ offset) for k in range(size)])


def after(array, block):
    return lax.optimization_barrier((array, block[3]))[0]


def exchange_order(size):
    return [1] + list(range(size - 1, 1, -1))


def exchange_tokens(tokens, norm_gain, key_weight, value_weight, break_bias, new_query):
    seq_count, piece, width = tokens.shape
    block_count = lax.axis_size("sp")
    share_count = lax.axis_size("tp")
    share = width // share_count
    own = lax.axis_index("sp")
    own_share = lax.axis_index("tp")
    bias_rows = jnp.transpose(break_bias, (0, 2, 1))
    columns = key_weight.shape[1]
    gain = norm_gain.reshape(1, width)
    query = lax.dynamic_slice_in_dim(new_query, own, 1, 0).astype(jnp.float32)

    def index_of(offset):
        return jnp.stack((own ^ offset, own_share)).astype(jnp.int32)

    order = exchange_order(block_count)
    arrived = {}
    bias_arrived = {}
    for offset in order:
        sent = lax.dynamic_slice(
            tokens, (own ^ offset, 0, own_share * share), (1, piece, share)
        ).reshape(piece, share)
        arrived[offset] = swap(sent, "sp", offset)
    for offset in order:
        bias_sent = lax.dynamic_index_in_dim(bias_rows, own ^ offset, 0, False)
        bias_arrived[offset] = swap(bias_sent, "sp", offset)
    built = {}
    built[0] = build_block(
        index_of(0),
        [tokens],
        gain,
        key_weight,
        value_weight,
        bias_rows,
        query,
        None,
        block_count,
    )
    latest = built[0]
    for place, offset in enumerate(order):
        shares = {0: arrived[offset]}
        if place != 1:
            shares[0] = after(shares[0], built[order[place - 2] if place else 0])
        bit = share_count // 2
        while bit:
            for known in list(shares):
                sent = shares[known]
                if known and place > 1:
                    sent = after(sent, latest)
                shares[known | bit] = swap(sent, "tp", bit)
            bit //= 2
        parts = [shares[k] for k in range(share_count)]
        latest = build_block(
            index_of(offset),
            parts,
            gain,
            key_weight,
            value_weight,
            bias_arrived[offset],
            query,
            latest[:2],
            block_count,
        )
        built[offset] = latest
    cache_pair, cache_bias = latest[:2]
    attended = jnp.zeros((1, columns), jnp.float32)
    for offset, block in built.items():
        beyond = jnp.zeros((1, columns), jnp.float32)
        for other, other_block in built.items():
            if other != offset:
                beyond = beyond + jnp.where((own ^ other) > (own ^ offset), other_block[3], 0.0)
        attended = attended + block[2] * jnp.exp(beyond)
    seq_index = lax.broadcasted_iota(jnp.int32, (seq_count, 1), 0)
    gathered = jnp.where(seq_index == own, attended, 0.0)
    for offset in order:
        gathered = jnp.where(seq_index == (own ^ offset), swap(attended, "sp", offset), gathered)
    return (cache_pair, jnp.transpose(cache_bias, (0, 2, 1))[None], gathered)


def local(tokens, norm_gain, key_weight, value_weight, break_bias, new_query):
    seq_count, _, width = tokens.shape
    block_count = lax.axis_size("sp")
    share_count = lax.axis_size("tp")
    paired = block_count & (block_count - 1) == 0 and share_count & (share_count - 1) == 0
    aligned = width % (128 * share_count) == 0
    whole_prompt = seq_count == block_count and block_count > 1
    body = exchange_tokens if paired and aligned and whole_prompt else exchange_rows
    return body(tokens, norm_gain, key_weight, value_weight, break_bias, new_query)


def solution(mesh):
    return jax.shard_map(
        local,
        mesh=mesh,
        in_specs=(
            P("grp", "sp", None),
            P(),
            P(None, "tp"),
            P(None, "tp"),
            P("grp", "sp", "tp"),
            P("grp", "tp"),
        ),
        out_specs=(
            P(("grp", "sp"), None, None, None, "tp"),
            P(("grp", "sp"), None, None, "tp"),
            P("grp", "tp"),
        ),
        check_vma=False,
    )
```

```python
import functools

import jax
import jax.numpy as jnp
from jax import lax
from jax.experimental import pallas as pl
from jax.experimental.pallas import tpu as pltpu
from jax.sharding import PartitionSpec as P

norm_eps = 1e-06


def normalize(tokens, norm_gain):
    widened = tokens.astype(jnp.float32)
    inverse = lax.rsqrt(jnp.mean(widened * widened, axis=-1, keepdims=True) + norm_eps)
    return (widened * inverse * norm_gain.astype(jnp.float32)).astype(jnp.bfloat16)


def project(flat_rows, key_weight, value_weight):
    key_rows = jnp.dot(flat_rows, key_weight, preferred_element_type=jnp.float32).astype(
        jnp.bfloat16
    )
    value_rows = jnp.dot(flat_rows, value_weight, preferred_element_type=jnp.float32).astype(
        jnp.bfloat16
    )
    return (key_rows, value_rows)


def read_placed(new_query, key_rows, value_rows, bias_rows, seq_count):
    block_count, piece, heads_here = bias_rows.shape
    columns = key_rows.shape[2]
    head_size = columns // heads_here
    span = block_count // seq_count
    own_index = lax.axis_index("sp")
    own_seq = own_index // span
    own_part = own_index % span
    own_query = lax.dynamic_slice_in_dim(new_query, own_seq, 1, 0).reshape(heads_here, head_size)
    key_heads = key_rows.reshape(block_count, piece, heads_here, head_size)
    logits = jnp.einsum("hd,nphd->nph", own_query, key_heads, preferred_element_type=jnp.float32)
    logits = logits * head_size ** (-0.5) + bias_rows.astype(jnp.float32)
    keep_log = jax.nn.log_sigmoid(-logits)
    block_totals = jnp.sum(keep_log, axis=1)
    own_slot = (jnp.arange(block_count, dtype=jnp.int32) == own_index)[:, None, None]
    placed = jnp.where(own_slot, block_totals[None], 0.0)
    gathered = lax.psum(placed, "sp")
    same_prompt = lax.dynamic_slice_in_dim(gathered, own_seq * span, span, 0)
    ordered = jnp.transpose(same_prompt, (1, 0, 2)).reshape(block_count * span, heads_here)
    beyond = lax.cumsum(ordered, axis=0, reverse=True) - ordered
    beyond = beyond.reshape(block_count, span, heads_here)
    carried = lax.dynamic_slice_in_dim(beyond, own_part, 1, 1)[:, 0, :]
    later_sum = lax.cumsum(keep_log, axis=1, reverse=True) - keep_log + carried[:, None, :]
    stick_weights = jnp.exp(jax.nn.log_sigmoid(logits) + later_sum).astype(jnp.bfloat16)
    value_heads = value_rows.reshape(block_count, piece, heads_here, head_size)
    mixed = jnp.einsum(
        "nph,nphd->hd", stick_weights, value_heads, preferred_element_type=jnp.float32
    )
    chosen = (jnp.arange(seq_count, dtype=jnp.int32) == own_seq)[:, None]
    partial_rows = jnp.where(chosen, mixed.reshape(1, columns), 0.0)
    return lax.psum(partial_rows, "sp")


def exchange_rows(tokens, norm_gain, key_weight, value_weight, break_bias, new_query):
    seq_count, tok_rows, width = tokens.shape
    heads_here = break_bias.shape[2]
    block_count = lax.axis_size("sp")
    piece = tok_rows * seq_count // block_count
    columns = key_weight.shape[1]
    normed = normalize(tokens, norm_gain)
    bias_pieces = break_bias.reshape(block_count, piece, heads_here)
    key_rows, value_rows = project(normed.reshape(-1, width), key_weight, value_weight)
    stacked_rows = jnp.stack((key_rows, value_rows), axis=1).reshape(block_count, piece, 2, columns)
    paired, bias_arrived = (
        lax.all_to_all(stacked_rows, "sp", split_axis=0, concat_axis=0, tiled=True),
        lax.all_to_all(bias_pieces, "sp", split_axis=0, concat_axis=0, tiled=True),
    )
    key_rows = paired[:, :, 0]
    value_rows = paired[:, :, 1]
    attended = read_placed(new_query, key_rows, value_rows, bias_arrived, seq_count)
    return (paired[None], bias_arrived[None], attended)


def block_kernel(part_count, whole_rows, carried, *refs):
    index_ref = refs[0]
    parts = refs[1 : 1 + part_count]
    gain_ref, key_ref, value_ref, query_ref = refs[1 + part_count : 5 + part_count]
    after_query = 5 + part_count
    bias_ref = None if carried else refs[after_query]
    rest = refs[after_query + (2 if carried else 1) :]
    cache_ref, bias_out_ref, partial_ref, total_ref = rest[:4]
    normed_ref, key_local, value_local, weight_sems = rest[4:]
    key_copy = pltpu.make_async_copy(key_ref, key_local, weight_sems.at[0])
    value_copy = pltpu.make_async_copy(value_ref, value_local, weight_sems.at[1])
    key_copy.start()
    value_copy.start()
    piece, width = normed_ref.shape
    heads_here = bias_out_ref.shape[-2]
    columns = key_ref.shape[1]
    head_size = columns // heads_here
    gain = gain_ref[...].astype(jnp.float32)
    if whole_rows:
        widened = parts[0][0].astype(jnp.float32)
        square_sum = jnp.sum(widened * widened, axis=-1, keepdims=True)
        inverse = lax.rsqrt(square_sum * (1.0 / width) + norm_eps)
        normed_ref[...] = (widened * inverse * gain).astype(jnp.bfloat16)
    else:
        share = width // part_count
        square_sum = jnp.zeros((piece, 1), jnp.float32)
        for part in parts:
            widened = part[:piece].astype(jnp.float32)
            square_sum = square_sum + jnp.sum(widened * widened, axis=-1, keepdims=True)
        inverse = lax.rsqrt(square_sum * (1.0 / width) + norm_eps)
        for offset, part in enumerate(parts):
            start = pl.multiple_of((index_ref[1] ^ offset) * share, share)
            own_gain = gain_ref[:, pl.ds(start, share)].astype(jnp.float32)
            scaled = part[:piece].astype(jnp.float32) * inverse * own_gain
            normed_ref[:, pl.ds(start, share)] = scaled.astype(jnp.bfloat16)
    normed = normed_ref[...]
    key_copy.wait()
    key_rows = jnp.dot(normed, key_local[...], preferred_element_type=jnp.float32).astype(
        jnp.bfloat16
    )
    value_copy.wait()
    value_rows = jnp.dot(normed, value_local[...], preferred_element_type=jnp.float32).astype(
        jnp.bfloat16
    )
    cache_ref[0, 0] = jnp.stack((key_rows, value_rows), axis=1)
    if carried:
        bias = parts[0][piece:, :piece].astype(jnp.float32)[:heads_here]
    else:
        bias = bias_ref[0].astype(jnp.float32)
    bias_out_ref[0] = bias.astype(jnp.bfloat16)
    head_of_row = lax.broadcasted_iota(jnp.int32, (heads_here, columns), 0)
    head_of_column = lax.broadcasted_iota(jnp.int32, (heads_here, columns), 1) // head_size
    own_head = head_of_row == head_of_column
    query = jnp.where(own_head, query_ref[...], 0.0).astype(jnp.bfloat16)
    logits = lax.dot_general(
        query, key_rows, (((1,), (1,)), ((), ())), preferred_element_type=jnp.float32
    )
    logits = logits * head_size ** (-0.5) + bias
    soft = jnp.log1p(jnp.exp(-jnp.abs(logits)))
    keep_log = jnp.minimum(-logits, 0.0) - soft
    break_log = jnp.minimum(logits, 0.0) - soft
    earlier = lax.broadcasted_iota(jnp.int32, (piece, piece), 1)
    later = lax.broadcasted_iota(jnp.int32, (piece, piece), 0) > earlier
    later_sum = jnp.dot(
        keep_log,
        later.astype(jnp.float32),
        preferred_element_type=jnp.float32,
        precision=lax.Precision.HIGHEST,
    )
    weights = jnp.exp(break_log + later_sum).astype(jnp.bfloat16)
    mixed = jnp.dot(weights, value_rows, preferred_element_type=jnp.float32)
    partial_ref[...] = jnp.sum(jnp.where(own_head, mixed, 0.0), axis=0, keepdims=True)
    totals = jnp.sum(keep_log, axis=1, keepdims=True)
    total_ref[...] = jnp.sum(jnp.where(own_head, totals, 0.0), axis=0, keepdims=True)


def build_block(index, parts, gain, key_weight, value_weight, bias, query, carried):
    whole_rows = parts[0].ndim == 3
    width, columns = key_weight.shape
    block_count, heads_here, piece = bias.shape
    part_count = len(parts)

    def full(array):
        return pl.BlockSpec(array.shape, lambda g, s: (0,) * array.ndim)

    if whole_rows:
        part_specs = [pl.BlockSpec((1, piece, width), lambda g, s: (s[0], 0, 0))]
    else:
        part_specs = [full(part) for part in parts]
    operands = [index, *parts, gain, key_weight, value_weight, query]
    in_place = pl.BlockSpec(memory_space=pl.ANY)
    specs = part_specs + [full(gain), in_place, in_place, full(query)]
    aliases = {}
    if carried is None:
        operands.append(bias)
        specs.append(pl.BlockSpec((1, heads_here, piece), lambda g, s: (s[0], 0, 0)))
    else:
        aliases = {len(operands): 0, len(operands) + 1: 1}
        operands += list(carried)
        specs += [in_place] * 2
    row = jax.ShapeDtypeStruct((1, columns), jnp.float32)
    return pl.pallas_call(
        functools.partial(block_kernel, part_count, whole_rows, carried is not None),
        grid_spec=pltpu.PrefetchScalarGridSpec(
            num_scalar_prefetch=1,
            grid=(1,),
            in_specs=specs,
            out_specs=[
                pl.BlockSpec((1, 1, piece, 2, columns), lambda g, s: (0, s[0], 0, 0, 0)),
                pl.BlockSpec((1, heads_here, piece), lambda g, s: (s[0], 0, 0)),
                pl.BlockSpec((1, columns), lambda g, s: (0, 0)),
                pl.BlockSpec((1, columns), lambda g, s: (0, 0)),
            ],
            scratch_shapes=[
                pltpu.VMEM((piece, width), jnp.bfloat16),
                pltpu.VMEM((width, columns), jnp.bfloat16),
                pltpu.VMEM((width, columns), jnp.bfloat16),
                pltpu.SemaphoreType.DMA((2,)),
            ],
        ),
        out_shape=[
            jax.ShapeDtypeStruct((1, block_count, piece, 2, columns), jnp.bfloat16),
            jax.ShapeDtypeStruct((block_count, heads_here, piece), jnp.bfloat16),
            row,
            row,
        ],
        input_output_aliases=aliases,
        compiler_params=pltpu.CompilerParams(vmem_limit_bytes=24 * 1024 * 1024),
        cost_estimate=pl.CostEstimate(
            flops=4 * piece * width * columns,
            transcendentals=3 * heads_here * piece,
            bytes_accessed=4 * width * columns + 2 * piece * (width + 2 * columns),
        ),
    )(*operands)


bias_tile = 16


def swap(array, axis, offset):
    size = lax.axis_size(axis)
    return lax.ppermute(array, axis, [(k, k ^ offset) for k in range(size)])


def after(array, block):
    return lax.optimization_barrier((array, block[3]))[0]


def exchange_order(size):
    return [1] + list(range(size - 1, 1, -1))


def exchange_tokens(tokens, norm_gain, key_weight, value_weight, break_bias, new_query):
    seq_count, piece, width = tokens.shape
    block_count = lax.axis_size("sp")
    share_count = lax.axis_size("tp")
    share = width // share_count
    own = lax.axis_index("sp")
    own_share = lax.axis_index("tp")
    bias_rows = jnp.transpose(break_bias, (0, 2, 1))
    heads_here = bias_rows.shape[1]
    columns = key_weight.shape[1]
    gain = norm_gain.reshape(1, width)
    query = lax.dynamic_slice_in_dim(new_query, own, 1, 0).astype(jnp.float32)

    def index_of(offset):
        return jnp.stack((own ^ offset, own_share)).astype(jnp.int32)

    order = exchange_order(block_count)
    arrived = {}
    for offset in order:
        sent = lax.dynamic_slice(
            tokens, (own ^ offset, 0, own_share * share), (1, piece, share)
        ).reshape(piece, share)
        bias_sent = lax.dynamic_index_in_dim(bias_rows, own ^ offset, 0, False)
        bias_sent = jnp.pad(bias_sent, ((0, bias_tile - heads_here), (0, share - piece)))
        sent = jnp.concatenate((sent, bias_sent), axis=0)
        arrived[offset] = swap(sent, "sp", offset)
    built = {}
    built[0] = build_block(
        index_of(0),
        [tokens],
        gain,
        key_weight,
        value_weight,
        bias_rows,
        query,
        None,
    )
    latest = built[0]
    for place, offset in enumerate(order):
        shares = {0: arrived[offset]}
        if place > 1:
            shares[0] = after(shares[0], built[order[place - 2]])
        bit = share_count // 2
        while bit:
            for known in list(shares):
                sent = shares[known]
                if known and place > 1:
                    sent = after(sent, latest)
                shares[known | bit] = swap(sent, "tp", bit)
            bit //= 2
        parts = [shares[k] for k in range(share_count)]
        latest = build_block(
            index_of(offset),
            parts,
            gain,
            key_weight,
            value_weight,
            bias_rows,
            query,
            latest[:2],
        )
        built[offset] = latest
    cache_pair, cache_bias = latest[:2]
    attended = jnp.zeros((1, columns), jnp.float32)
    for offset, block in built.items():
        beyond = jnp.zeros((1, columns), jnp.float32)
        for other, other_block in built.items():
            if other != offset:
                beyond = beyond + jnp.where((own ^ other) > (own ^ offset), other_block[3], 0.0)
        attended = attended + block[2] * jnp.exp(beyond)
    seq_index = lax.broadcasted_iota(jnp.int32, (seq_count, 1), 0)
    gathered = jnp.where(seq_index == own, attended, 0.0)
    for offset in order:
        gathered = jnp.where(seq_index == (own ^ offset), swap(attended, "sp", offset), gathered)
    return (cache_pair, jnp.transpose(cache_bias, (0, 2, 1))[None], gathered)


def local(tokens, norm_gain, key_weight, value_weight, break_bias, new_query):
    seq_count, _, width = tokens.shape
    block_count = lax.axis_size("sp")
    share_count = lax.axis_size("tp")
    paired = block_count & (block_count - 1) == 0 and share_count & (share_count - 1) == 0
    aligned = width % (128 * share_count) == 0
    whole_prompt = seq_count == block_count and block_count > 1
    whole_prompt = whole_prompt and tokens.shape[1] <= width // share_count
    whole_prompt = whole_prompt and break_bias.shape[2] <= bias_tile
    body = exchange_tokens if paired and aligned and whole_prompt else exchange_rows
    return body(tokens, norm_gain, key_weight, value_weight, break_bias, new_query)


def solution(mesh):
    return jax.shard_map(
        local,
        mesh=mesh,
        in_specs=(
            P("grp", "sp", None),
            P(),
            P(None, "tp"),
            P(None, "tp"),
            P("grp", "sp", "tp"),
            P("grp", "tp"),
        ),
        out_specs=(
            P(("grp", "sp"), None, None, None, "tp"),
            P(("grp", "sp"), None, None, "tp"),
            P("grp", "tp"),
        ),
        check_vma=False,
    )
```
